32 devices in a mesh: ep: 4 (over y, x), tp: 8 (over z, core).
Axes of the slice: x: 2, y: 2, z: 4, core: 2. Of those that a mesh axis runs over, the one named last changes fastest.
Arguments:
- tokens: bfloat16 [256, 2048], P('ep', 'tp'), may hold values from -6 to 6
- prior_state: float32 [256, 16, 64, 128], P('ep', 'tp'), may hold values from -3 to 3
- decay_rate: float32 [16], P('tp'), may hold values from 0.01 to 0.5
- norm_in: float32 [2048], replicated, may hold values from 0.1 to 1.9
- query_weight: bfloat16 [2048, 1024], P(None, 'tp'), may hold values from -0.125 to 0.125
- key_weight: bfloat16 [2048, 1024], P(None, 'tp'), may hold values from -0.125 to 0.125
- value_weight: bfloat16 [2048, 2048], P(None, 'tp'), may hold values from -0.125 to 0.125
- gate_weight: bfloat16 [2048, 2048], P(None, 'tp'), may hold values from -0.125 to 0.125
- out_weight: bfloat16 [2048, 2048], P('tp'), may hold values from -0.125 to 0.125
- norm_moe: float32 [2048], replicated, may hold values from 0.1 to 1.9
- routes: int32 [256, 2], replicated, may hold values from 0 to 3, all different within a row; in each aligned block of 64 rows (0 to 63, 64 to 127, ...) at most 48 rows name the same one
- route_weight: float32 [256, 2], replicated, may hold values from 0.1 to 1
- expert_gate: bfloat16 [4, 2048, 7168], P('ep', None, 'tp'), may hold values from -0.125 to 0.125
- expert_up: bfloat16 [4, 2048, 7168], P('ep', None, 'tp'), may hold values from -0.125 to 0.125
- expert_down: bfloat16 [4, 7168, 2048], P('ep', 'tp'), may hold values from -0.0625 to 0.0625
Outputs:
- next_hidden: bfloat16 [256, 2048], P('ep', 'tp')
- new_state: float32 [256, 16, 64, 128], P('ep', 'tp')
The draws below stay inside these ranges and needn't reach their ends.
Inputs may be any that keep to these rules, and one draw needn't show every extreme that they name: `routes`: the 2 experts of a row differ. In each aligned block of 64 rows (the sequences of one index of ep), no expert is named by more than 48 rows, a bound that some block reaches.
All inputs are finite; a program needn't handle non-finite values.
Results may differ from the reference program's by a relative error of at most 0.011.
Values may be sent and summed in bfloat16 or wider, within the bound.
A program may use at most 64 MiB of HBM per device.

```python
import math
import jax
import jax.numpy as jnp
import numpy as np
from jax import lax

D = 2048
HEADS = 16
DK = 64
DV = 128
FFE = 7168
TOP_K = 2
SEQ_DEV = 64
EXPERTS = 4
CAP = 48
BATCH = 256
HK = 1024
HV = 2048
N_EP = 4


def block_levels(key, dims, shards, low, top_value):
    factor_of = 1.0
    for axis_at, parts in shards:
        steps = jax.random.uniform(jax.random.fold_in(jax.random.fold_in(key, 6), axis_at), (parts,), jnp.float32, low / len(shards), top_value / len(shards))
        factor_of = factor_of * jnp.repeat(jnp.exp(steps), dims[axis_at] // parts).reshape((-1,) + (1,) * (len(dims) - 1 - axis_at))
    return factor_of


def routed_block(stream_key, own, number, rows, amount, top, reach, slope):
    order = jax.random.permutation(stream_key, amount)
    packed, ordinary = shares(amount, rows * top, reach, slope, True), shares(amount, rows * top, reach, slope, False)
    places = jnp.arange(amount)

    def named(lengths, offset_by):
        used = int((lengths > 0).sum())
        fixed = max(1, used // 4)
        passed = fixed + (places - fixed + offset_by * (used - fixed)) % max(1, amount - fixed)
        return jnp.zeros((amount,), jnp.int32).at[order[jnp.where(places < fixed, places, passed)]].set(jnp.asarray(lengths, jnp.int32))

    lengths = jnp.where(number % 4 == 0, named(packed, number // 4), named(ordinary, number - number // 4 - 1))
    mixed = jax.random.permutation(jax.random.fold_in(own, 3), amount)
    giver, sink = mixed[0:amount // 2 * 2:2], mixed[1:amount // 2 * 2:2]
    slack = jnp.minimum(lengths[giver] - 1, reach - lengths[sink]) // 2
    slack = jnp.where((giver == order[0]) | (sink == order[0]) | (lengths[sink] == 0), 0, jnp.maximum(slack, 0))
    passed = jax.random.randint(jax.random.fold_in(own, 4), (amount // 2,), 0, 1 << 20) % (slack + 1)
    lengths = lengths.at[giver].add(-passed).at[sink].add(passed)
    items = jnp.searchsorted(jnp.cumsum(lengths), jnp.arange(rows * top), side="right").astype(jnp.int32)
    listing = items.reshape(top, rows).T
    listing = listing[jax.random.permutation(jax.random.fold_in(own, 1), rows)]
    offset_by = jax.random.randint(jax.random.fold_in(own, 2), (rows, 1), 0, top)
    return jnp.take_along_axis(listing, (jnp.arange(top)[None, :] + offset_by) % top, axis=1)


def shares(number_of, total, limit, skew, full):
    portions = [(1 << 20) // math.isqrt(grade ** skew) + 1 for grade in range(1, number_of + 1)]
    largest = limit if full else min(limit, max(-(-total // number_of), total * portions[0] // sum(portions)))
    least = 1 if total - largest >= number_of - 1 else 0
    counts, surplus = [largest] + [least] * (number_of - 1), total - largest - least * (number_of - 1)
    while surplus > 0:
        free = [i for i in range(1, number_of) if counts[i] < largest] or [i for i in range(1, number_of) if counts[i] < limit]
        whole, budget = sum([portions[i] for i in free]), surplus
        for i in free:
            more = min(limit - counts[i], max(1, budget * portions[i] // whole), surplus)
            counts[i] = counts[i] + more
            surplus = surplus - more
    return np.array(counts)


def noise(key, dims, spread, limit, shards=(), kind=jnp.bfloat16):
    drawn = jax.random.normal(key, dims, jnp.float32) * spread
    if len(shards) > 0:
        drawn = block_levels(key, dims, shards, -0.22, 0.18) * drawn
    return jnp.clip(drawn, min=-limit, max=limit).astype(kind)


def setup_inputs(seed: int = 0) -> dict:
    keys = jax.random.split(jax.random.key(seed), 16)
    tokens = noise(keys[0], (BATCH, D), 1.0, 6.0, ((0, 4), (1, 8)))
    prior_state = noise(keys[1], (BATCH, HEADS, DK, DV), 0.5, 3.0, ((0, 4), (1, 8)), jnp.float32)
    decay_rate = jnp.clip(jnp.exp(math.log(0.5) - 3.912023 * jax.random.uniform(keys[2], (HEADS,), jnp.float32) ** block_levels(keys[2], (HEADS,), ((0, 8),), -0.2, 0.2)), 0.01, 0.5)
    norm_in = jnp.clip(1.0 + 0.18 * jax.random.normal(keys[3], (D,), jnp.float32), 0.1, 1.9)
    query_weight = noise(keys[4], (D, HK), D ** -0.5, 0.125, ((1, 8),))
    key_weight = noise(keys[5], (D, HK), D ** -0.5, 0.125, ((1, 8),))
    value_weight = noise(keys[6], (D, HV), D ** -0.5, 0.125, ((1, 8),))
    gate_weight = noise(keys[7], (D, HV), D ** -0.5, 0.125, ((1, 8),))
    out_weight = noise(keys[8], (HV, D), HV ** -0.5, 0.125, ((0, 8),))
    norm_moe = jnp.clip(1.0 + 0.18 * jax.random.normal(keys[9], (D,), jnp.float32), 0.1, 1.9)
    routes_keys = jax.random.split(jax.random.fold_in(keys[10], 1), BATCH // SEQ_DEV)
    routes_turns = jax.random.permutation(jax.random.fold_in(keys[10], 3), BATCH // SEQ_DEV)
    routes = jax.vmap(lambda own, number: routed_block(jax.random.fold_in(keys[10], 2), own, number, SEQ_DEV, EXPERTS, TOP_K, CAP, 2))(routes_keys, routes_turns).reshape((BATCH, TOP_K))
    route_weight = jnp.clip(jax.random.uniform(keys[11], (BATCH, TOP_K), jnp.float32, 0.1, 1.0), 0.1, 1.0)
    expert_gate = noise(keys[12], (EXPERTS, D, FFE), D ** -0.5, 0.125, ((0, 4), (2, 8)))
    expert_up = noise(keys[13], (EXPERTS, D, FFE), D ** -0.5, 0.125, ((0, 4), (2, 8)))
    expert_down = noise(keys[14], (EXPERTS, FFE, D), FFE ** -0.5, 0.0625, ((0, 4), (1, 8)))
    return dict(tokens=tokens, prior_state=prior_state, decay_rate=decay_rate, norm_in=norm_in, query_weight=query_weight, key_weight=key_weight, value_weight=value_weight, gate_weight=gate_weight, out_weight=out_weight, norm_moe=norm_moe, routes=routes, route_weight=route_weight, expert_gate=expert_gate, expert_up=expert_up, expert_down=expert_down)


EPSILON = 1e-06

def rms_scale(row_block, gain_row):
    values = row_block.astype(jnp.float32)
    factor = lax.rsqrt(lax.optimization_barrier(jnp.mean(values * values, -1, keepdims=True)) + EPSILON)
    return (values * factor * gain_row).astype(jnp.bfloat16)

def project(normed_in, weight):
    stored = jnp.dot(normed_in, weight, preferred_element_type=jnp.float32).astype(jnp.bfloat16)
    return lax.optimization_barrier(stored).astype(jnp.float32)

def reference(tokens, prior_state, decay_rate, norm_in, query_weight, key_weight, value_weight, gate_weight, out_weight, norm_moe, routes, route_weight, expert_gate, expert_up, expert_down):
    total = tokens.shape[0]
    normed_in = rms_scale(tokens, norm_in)
    query = project(normed_in, query_weight).reshape(total, HEADS, DK)
    keyed = project(normed_in, key_weight).reshape(total, HEADS, DK) * DK ** (-0.5)
    valued = project(normed_in, value_weight).reshape(total, HEADS, DV)
    gate_pre = project(normed_in, gate_weight)
    keep = (1.0 - decay_rate)[None, :, None, None]
    new_state = keep * prior_state + jnp.einsum('bhk,bhv->bhkv', keyed, valued, precision=lax.Precision.HIGHEST)
    read = jnp.einsum('bhk,bhkv->bhv', query, new_state, precision=lax.Precision.HIGHEST)
    centred = read - lax.optimization_barrier(jnp.mean(read, -1, keepdims=True))
    normed = centred * lax.rsqrt(lax.optimization_barrier(jnp.mean(centred * centred, -1, keepdims=True)) + EPSILON)
    mixed_heads = (jax.nn.silu(gate_pre) * normed.reshape(total, HEADS * DV)).astype(jnp.bfloat16)
    mixer_out = jnp.dot(mixed_heads, out_weight, preferred_element_type=jnp.float32)
    resid = (tokens.astype(jnp.float32) + mixer_out).astype(jnp.bfloat16)
    expert_in = rms_scale(resid, norm_moe)
    slot_count = N_EP * CAP
    slot_ids = jnp.arange(slot_count, dtype=jnp.int32)

    def one_expert(carry, pack):
        label, gate_w, up_w, down_w = pack
        match = routes == label
        chosen = lax.optimization_barrier(jnp.sum(match.astype(jnp.int32), 1)).astype(jnp.int32)
        weighted = lax.optimization_barrier(jnp.sum(jnp.where(match, route_weight, 0.0), 1))
        rank = jnp.cumsum(chosen).astype(jnp.int32) - chosen
        place = ((rank[:, None] == slot_ids[None, :]) & (chosen[:, None] > 0)).astype(jnp.float32)
        rows_in = jnp.dot(place.T.astype(jnp.bfloat16), expert_in, preferred_element_type=jnp.float32).astype(jnp.bfloat16)
        gate_part = jnp.dot(rows_in, gate_w, preferred_element_type=jnp.float32)
        up_part = jnp.dot(rows_in, up_w, preferred_element_type=jnp.float32)
        hidden = (jax.nn.silu(gate_part) * up_part).astype(jnp.bfloat16)
        down = jnp.dot(hidden, down_w, preferred_element_type=jnp.float32)
        carry = carry + jnp.dot(place * weighted[:, None], down, precision=lax.Precision.HIGHEST)
        return (carry, None)
    start = jnp.zeros((total, D), jnp.float32)
    labels = jnp.arange(EXPERTS, dtype=jnp.int32)
    moe_sum, unused = lax.scan(one_expert, start, (labels, expert_gate, expert_up, expert_down))
    next_hidden = (resid.astype(jnp.float32) + moe_sum).astype(jnp.bfloat16)
    return (next_hidden, new_state)
```

```python
import functools
import math

import jax
import jax.numpy as jnp
from jax import lax
from jax.experimental import pallas as pl
from jax.experimental.pallas import tpu as pltpu
from jax.sharding import PartitionSpec as P

EPSILON = 1e-06
MESH = pl.DeviceIdType.MESH
F32 = jnp.float32
BF16 = jnp.bfloat16
GROUP = 8


def dot(a, b):
    return jnp.dot(a, b, preferred_element_type=F32)


def kernel(
    nz, groups, cap, dk, dv,
    tokens, state_hbm, decay, norm_in, wq, wk, wv, wg, wo, norm_moe, routes, rweight, eg, eu, ed,
    out_hidden, out_state,
    tok_full, xn, wqk_v, wv_v, wg_v, wo_v, eg_v, eu_v, ed_v, st, kt, vv, qv, kv, read_v,
    rs1s, rs1r, rs2s, rs2r, res_full, disp_s, xin, accg, accu, dn1s, dn1r, dn2s, ret,
    fin_s, fin_r, place_v, sphi, splo,
    load_sem, state_sem,
    agz_s, agz_r, agp_s, agp_r, rs1_s, rs1_r, rs2_s, rs2_r, ar_s, ar_r,
    dp_s, dp_r, fw_s, fw_r, dn_s, dn_r, rt_s, rt_r, fn_s, fn_r,
):
    rows, width = tokens.shape
    full = xn.shape[1]
    hk = wqk_v.shape[1] // 2
    heads = st.shape[1]
    slots = groups * cap
    e = lax.axis_index("ep")
    t = lax.axis_index("tp")
    z = t // 2
    c = lax.rem(t, 2)
    oc = 1 - c
    partner = t + 1 - 2 * c

    if wq.shape[1] == hk:
        queries = [
            pltpu.make_async_copy(wq, wqk_v.at[:, pl.ds(0, hk)], load_sem.at[0]),
            pltpu.make_async_copy(wk, wqk_v.at[:, pl.ds(hk, hk)], load_sem.at[8]),
        ]
    else:
        queries = [pltpu.make_async_copy(wq, wqk_v, load_sem.at[0])]
    loads = [
        pltpu.make_async_copy(wv, wv_v, load_sem.at[2]),
        pltpu.make_async_copy(wg, wg_v, load_sem.at[3]),
        pltpu.make_async_copy(state_hbm, st, state_sem),
        pltpu.make_async_copy(wo, wo_v, load_sem.at[4]),
        pltpu.make_async_copy(eg.at[0], eg_v, load_sem.at[5]),
        pltpu.make_async_copy(eu.at[0], eu_v, load_sem.at[6]),
        pltpu.make_async_copy(ed.at[0], ed_v, load_sem.at[7]),
    ]
    for load in queries + loads:
        load.start()

    barrier = pltpu.get_barrier_semaphore()
    pl.semaphore_signal(barrier, inc=1, device_id={"tp": partner}, device_id_type=MESH)
    for d in range(1, nz):
        peer = 2 * lax.rem(z + d, nz) + c
        pl.semaphore_signal(barrier, inc=1, device_id={"tp": peer}, device_id_type=MESH)
    for d in range(1, groups):
        pl.semaphore_signal(
            barrier, inc=1, device_id={"ep": lax.rem(e + d, groups)}, device_id_type=MESH
        )
    pl.semaphore_wait(barrier, nz + groups - 1)

    started = []

    def remote(src, dst, ssem, rsem, where):
        return pltpu.make_async_remote_copy(
            src_ref=src, dst_ref=dst, send_sem=ssem, recv_sem=rsem,
            device_id=where, device_id_type=MESH,
        )

    def send(*args):
        copy = remote(*args)
        copy.start()
        started.append(copy)

    def zpeer(d):
        return {"tp": 2 * lax.rem(z + d, nz) + c}

    def zat(d):
        return lax.rem(z + nz + d, nz)

    def epeer(d):
        return {"ep": lax.rem(e + d, groups)}

    def cols(slot):
        return pl.ds(pl.multiple_of(slot * width, width), width)

    pair = {"tp": partner}

    for d in range(1, nz):
        send(tokens, tok_full.at[t], agz_s.at[d], agz_r.at[d], zpeer(d))
    send(tokens, tok_full.at[t], agp_s.at[0], agp_r.at[0], pair)
    tok_full[t] = tokens[...]

    total = routes.shape[1]
    at_row = lax.broadcasted_iota(jnp.int32, (rows, total), 0) + e * rows
    own = at_row == lax.broadcasted_iota(jnp.int32, (rows, total), 1)

    def column(ref, k):
        line = ref[pl.ds(k, 1), :].astype(F32)
        return jnp.sum(jnp.where(own, line, 0.0), 1, keepdims=True)

    padded = -(-slots // 128) * 128
    index = lax.broadcasted_iota(jnp.int32, (rows, padded), 1).astype(F32)
    label = jnp.floor((index + 0.5) / cap)
    place_at = index - label * cap
    chosen = jnp.zeros((rows, padded), F32)
    weight = jnp.zeros((rows, padded), F32)
    for k in range(routes.shape[0]):
        same = column(routes, k) == label
        chosen = jnp.where(same, 1.0, chosen)
        weight = jnp.where(same, column(rweight, k), weight)
    lower = lax.broadcasted_iota(jnp.int32, (rows, rows), 0) > lax.broadcasted_iota(
        jnp.int32, (rows, rows), 1
    )
    rank = dot(jnp.where(lower, 1.0, 0.0).astype(BF16), chosen.astype(BF16))
    hit = jnp.where(rank == place_at, chosen, 0.0)
    spread = (weight * hit)[:, :slots]
    high = spread.astype(BF16)
    sphi[...] = high
    splo[...] = (spread - high.astype(F32)).astype(BF16)
    place_v[...] = jnp.transpose(hit)[:slots].astype(BF16)

    for d in range(1, nz):
        slot = tok_full.at[2 * zat(-d) + c]
        remote(tokens, slot, agz_s.at[d], agz_r.at[d], zpeer(d)).wait_recv()
        send(slot, slot, agp_s.at[d], agp_r.at[d], pair)
    for d in range(nz):
        slot = tok_full.at[2 * zat(-d) + oc]
        remote(tokens, slot, agp_s.at[d], agp_r.at[d], pair).wait_recv()

    square = jnp.zeros((rows, 1), F32)
    for s in range(2 * nz):
        x = tok_full[s].astype(F32)
        square += jnp.sum(x * x, 1, keepdims=True)
    factor = lax.rsqrt(square / full + EPSILON)
    for s in range(2 * nz):
        x = tok_full[s].astype(F32)
        gain = norm_in[:, pl.ds(s * width, width)]
        xn[:, pl.ds(s * width, width)] = (x * factor * gain).astype(BF16)
    for load in queries:
        load.wait()
    qk = dot(xn[...], wqk_v[...]).astype(BF16).astype(F32)
    scale = jnp.where(lax.broadcasted_iota(jnp.int32, (1, 2 * hk), 1) < hk, 1.0, dk ** (-0.5))
    qkt = jnp.transpose(qk * scale)
    for g in range(rows // GROUP):
        kt[g] = qkt[:, g * GROUP:(g + 1) * GROUP]
    loads[0].wait()
    vv[...] = dot(xn[...], wv_v[...]).astype(BF16).astype(F32)

    loads[2].wait()
    qv[...] = (qk * scale)[:, :hk]
    kv[...] = (qk * scale)[:, hk:]

    def read_rows(g, carry):
        base = pl.multiple_of(g * GROUP, GROUP)
        values = vv[pl.ds(base, GROUP), :]
        both = qv[pl.ds(base, GROUP), :] * kv[pl.ds(base, GROUP), :]
        parts = []
        for h in range(heads):
            keep = 1.0 - decay[h]
            lines = []
            for b in range(GROUP):
                qcol = kt[g, pl.ds(h * dk, dk), pl.ds(b, 1)]
                lines.append(jnp.sum(qcol * st[base + b, h], 0, keepdims=True))
            overlap = jnp.sum(both[:, h * dk:(h + 1) * dk], 1, keepdims=True)
            parts.append(
                keep * jnp.concatenate(lines, 0) + overlap * values[:, h * dv:(h + 1) * dv]
            )
        read_v[pl.ds(base, GROUP), :] = jnp.concatenate(parts, 1)
        return carry

    def update(g, carry):
        base = pl.multiple_of(g * GROUP, GROUP)
        values = vv[pl.ds(base, GROUP), :]
        for b in range(GROUP):
            for h in range(heads):
                keep = 1.0 - decay[h]
                kcol = kt[g, pl.ds(hk + h * dk, dk), pl.ds(b, 1)]
                vrow = values[b:b + 1, h * dv:(h + 1) * dv]
                out_state[base + b, h] = keep * st[base + b, h] + kcol * vrow
        return carry

    lax.fori_loop(0, rows // GROUP, read_rows, 0)

    loads[1].wait()
    gate_pre = dot(xn[...], wg_v[...]).astype(BF16).astype(F32)
    read = read_v[...]
    normed = []
    for h in range(heads):
        part = read[:, h * dv:(h + 1) * dv]
        part = part - jnp.mean(part, -1, keepdims=True)
        normed.append(part * lax.rsqrt(jnp.mean(part * part, -1, keepdims=True) + EPSILON))
    mixed = (jax.nn.silu(gate_pre) * jnp.concatenate(normed, 1)).astype(BF16)

    loads[3].wait()
    order = list(range(1, nz)) + [0]
    for d in order:
        rs1s[d] = dot(mixed, wo_v[:, cols(2 * zat(d) + oc)]).astype(BF16)
        send(rs1s.at[d], rs1r.at[d], rs1_s.at[d], rs1_r.at[d], pair)
    mixer = None
    for d in order:
        part = dot(mixed, wo_v[:, cols(2 * zat(d) + c)])
        remote(rs1s.at[d], rs1r.at[d], rs1_s.at[d], rs1_r.at[d], pair).wait_recv()
        part = part + rs1r[d].astype(F32)
        if d == 0:
            mixer = part
        else:
            rs2s[d] = part.astype(BF16)
            send(rs2s.at[d], rs2r.at[d], rs2_s.at[d], rs2_r.at[d], zpeer(d))
    for d in range(1, nz):
        remote(rs2s.at[d], rs2r.at[d], rs2_s.at[d], rs2_r.at[d], zpeer(d)).wait_recv()
        mixer += rs2r[d].astype(F32)
    resid = (tokens[...].astype(F32) + mixer).astype(BF16)
    res_full[0] = resid
    for d in range(1, nz):
        send(res_full.at[0], res_full.at[d], ar_s.at[d], ar_r.at[d], zpeer(d))

    def dispatch(i):
        if i > 0:
            remote(
                res_full.at[0], res_full.at[i], ar_s.at[i], ar_r.at[i], zpeer(i)
            ).wait_recv()
        moved = dot(place_v[...], res_full[i]).astype(BF16)
        for g in range(groups):
            disp_s[i, g] = moved[g * cap:(g + 1) * cap]
        for d in range(1, groups):
            send(
                disp_s.at[i, lax.rem(e + d, groups)], xin.at[c, i, d],
                dp_s.at[i * groups + d], dp_r.at[i * groups + d], epeer(d),
            )
        xin[c, i, 0] = disp_s[i, e]

    blocks = rows // GROUP
    dispatch(0)
    lax.fori_loop(0, blocks // 2, update, 0)
    for i in range(1, nz):
        dispatch(i)
    lax.fori_loop(blocks // 2, blocks, update, 0)

    def flat(x):
        return jnp.concatenate([x[g] for g in range(groups)], 0)

    loads[4].wait()
    loads[5].wait()
    square = jnp.zeros((slots, 1), F32)
    first = True
    steps = []
    for i in range(nz):
        steps.append((0, i))
        if i > 0:
            steps.append((1, i - 1))
    steps.append((1, nz - 1))
    for other, i in steps:
        where = oc if other else c
        if other:
            block = xin.at[where, i]
            remote(block, block, fw_s.at[i], fw_r.at[i], pair).wait_recv()
        else:
            for d in range(1, groups):
                k = i * groups + d
                remote(disp_s.at[i, 0], xin.at[c, i, d], dp_s.at[k], dp_r.at[k], epeer(d)).wait_recv()
            block = xin.at[where, i]
            send(block, block, fw_s.at[i], fw_r.at[i], pair)
        x = flat(xin[where, i]).astype(F32)
        square += jnp.sum(x * x, 1, keepdims=True)
        slot = cols(2 * zat(-i) + where)
        x = (x * norm_moe[:, slot]).astype(BF16)
        if first:
            accg[...] = dot(x, eg_v[slot, :])
            accu[...] = dot(x, eu_v[slot, :])
            first = False
        else:
            accg[...] += dot(x, eg_v[slot, :])
            accu[...] += dot(x, eu_v[slot, :])
    factor = lax.rsqrt(square / full + EPSILON)
    hidden = (jax.nn.silu(accg[...] * factor) * (accu[...] * factor)).astype(BF16)

    loads[6].wait()
    for d in order:
        part = dot(hidden, ed_v[:, cols(2 * zat(d) + oc)]).astype(BF16)
        for g in range(groups):
            dn1s[d, g] = part[g * cap:(g + 1) * cap]
        send(dn1s.at[d], dn1r.at[d], dn_s.at[d], dn_r.at[d], pair)
    for d in order:
        part = dot(hidden, ed_v[:, cols(2 * zat(d) + c)])
        remote(dn1s.at[d], dn1r.at[d], dn_s.at[d], dn_r.at[d], pair).wait_recv()
        for g in range(groups):
            dn2s[d, g] = (part[g * cap:(g + 1) * cap] + dn1r[d, g].astype(F32)).astype(BF16)
        for g in range(1, groups):
            k = d * groups + g
            send(
                dn2s.at[d, g], ret.at[d, e], rt_s.at[k], rt_r.at[k],
                {"ep": lax.rem(e + groups - g, groups)},
            )
        ret[d, e] = dn2s[d, 0]
    mine = None
    for d in order:
        for g in range(1, groups):
            k = d * groups + g
            remote(
                dn2s.at[d, g], ret.at[d, lax.rem(e + g, groups)], rt_s.at[k], rt_r.at[k],
                {"ep": lax.rem(e + groups - g, groups)},
            ).wait_recv()
        block = flat(ret[d])
        part = dot(sphi[...], block) + dot(splo[...], block)
        if d == 0:
            mine = part
        else:
            fin_s[d] = part.astype(BF16)
            send(fin_s.at[d], fin_r.at[d], fn_s.at[d], fn_r.at[d], zpeer(d))
    for d in range(1, nz):
        remote(fin_s.at[d], fin_r.at[d], fn_s.at[d], fn_r.at[d], zpeer(d)).wait_recv()
        mine += fin_r[d].astype(F32)
    out_hidden[...] = (res_full[0].astype(F32) + mine).astype(BF16)

    for copy in started:
        copy.wait_send()


def solution(mesh):
    groups = mesh.shape["ep"]
    nz = mesh.shape["tp"] // 2

    def on_device(
        tokens, prior_state, decay_rate, norm_in, query_weight, key_weight, value_weight,
        gate_weight, out_weight, norm_moe, routes, route_weight, expert_gate, expert_up, expert_down,
    ):
        rows, width = tokens.shape
        full = width * 2 * nz
        heads, dk, dv = prior_state.shape[1:]
        hk, hv = query_weight.shape[1], value_weight.shape[1]
        ff = expert_gate.shape[2]
        top = routes.shape[1]
        bound = (3 * top * rows + 2 * groups - 1) // (2 * groups)
        cap = -(-bound // 16) * 16
        slots = groups * cap
        if hk % 128:
            query_weight = jnp.concatenate([query_weight, key_weight], 1)
        room = 67043328 - 4 * math.prod(prior_state.shape) - 256 * 1024
        vm = pl.BlockSpec(memory_space=pltpu.VMEM)
        sm = pl.BlockSpec(memory_space=pltpu.SMEM)
        hb = pl.BlockSpec(memory_space=pltpu.HBM)
        slab = lambda: pltpu.VMEM((nz, rows, width), BF16)
        block = lambda: pltpu.VMEM((nz, groups, cap, width), BF16)
        dma = pltpu.SemaphoreType.DMA
        two = lambda n: [dma((n,)), dma((n,))]
        scratch = [
            pltpu.VMEM((2 * nz, rows, width), BF16),
            pltpu.VMEM((rows, full), BF16),
            pltpu.VMEM((full, 2 * hk), BF16),
            pltpu.VMEM((full, hv), BF16),
            pltpu.VMEM((full, hv), BF16),
            pltpu.VMEM((hv, full), BF16),
            pltpu.VMEM((full, ff), BF16),
            pltpu.VMEM((full, ff), BF16),
            pltpu.VMEM((ff, full), BF16),
            pltpu.VMEM(prior_state.shape, F32),
            pltpu.VMEM((rows // GROUP, 2 * hk, GROUP), F32),
            pltpu.VMEM((rows, hv), F32),
            pltpu.VMEM((rows, hk), F32),
            pltpu.VMEM((rows, hk), F32),
            pltpu.VMEM((rows, hv), F32),
            slab(), slab(), slab(), slab(), slab(),
            block(),
            pltpu.VMEM((2, nz, groups, cap, width), BF16),
            pltpu.VMEM((slots, ff), F32),
            pltpu.VMEM((slots, ff), F32),
            block(), block(), block(), block(),
            slab(), slab(),
            pltpu.VMEM((slots, rows), BF16),
            pltpu.VMEM((rows, slots), BF16),
            pltpu.VMEM((rows, slots), BF16),
            dma((9,)), dma,
            *two(nz), *two(nz), *two(nz), *two(nz), *two(nz),
            *two(nz * groups), *two(nz), *two(nz), *two(nz * groups), *two(nz),
        ]
        return pl.pallas_call(
            functools.partial(kernel, nz, groups, cap, dk, dv),
            out_shape=(
                pltpu.VMEM(tokens.shape, BF16),
                pltpu.VMEM(prior_state.shape, F32),
            ),
            in_specs=[vm, hb, sm, vm, hb, hb, hb, hb, hb, vm, vm, vm, hb, hb, hb],
            out_specs=(vm, vm),
            scratch_shapes=scratch,
            compiler_params=pltpu.CompilerParams(
                collective_id=0, has_side_effects=True, vmem_limit_bytes=room
            ),
        )(
            tokens, prior_state, decay_rate, norm_in.reshape(1, -1), query_weight, key_weight,
            value_weight, gate_weight, out_weight, norm_moe.reshape(1, -1), routes.T,
            route_weight.T, expert_gate, expert_up, expert_down,
        )

    placed = (
        P("ep", "tp"), P("ep", "tp", None, None), P("tp"), P(), P(None, "tp"), P(None, "tp"),
        P(None, "tp"), P(None, "tp"), P("tp", None), P(), P(), P(), P("ep", None, "tp"),
        P("ep", None, "tp"), P("ep", "tp", None),
    )
    return jax.shard_map(
        on_device,
        mesh=mesh,
        in_specs=placed,
        out_specs=(P("ep", "tp"), P("ep", "tp", None, None)),
        check_vma=False,
    )
```
